32 devices in a mesh: sp: 8 (over z, x), tp: 4 (over y, core).
Axes of the slice: x: 2, y: 2, z: 4, core: 2. Of those that a mesh axis runs over, the one named last changes fastest.
Arguments:
- hidden_in: bfloat16 [2048, 2048], P('sp'), may hold values from -6 to 6
- cotangent: bfloat16 [2048, 2048], P('sp'), may hold values from -6 to 6
- routes: int32 [2048, 2], P('sp'), may hold values from 0 to 7, all different within a row; in each aligned block of 256 rows (0 to 255, 256 to 511, ...) at most 96 rows name the same one
- routing_weights: float32 [2048, 2], P('sp'), may hold values from 0.1 to 1
- w_gate: bfloat16 [8, 2048, 1024], P('sp', None, 'tp'), may hold values from -0.125 to 0.125
- w_up: bfloat16 [8, 2048, 1024], P('sp', None, 'tp'), may hold values from -0.125 to 0.125
- w_down: bfloat16 [8, 1024, 2048], P('sp', 'tp'), may hold values from -0.1875 to 0.1875
- b_gate: bfloat16 [2048, 1024], P('sp', 'tp'), may hold values from -6 to 6
- c_gate: bfloat16 [2048, 1024], P('sp', 'tp'), may hold values from -6 to 6
- x_in: bfloat16 [2048, 1024], P('sp', 'tp'), may hold values from -6 to 6
- taps: bfloat16 [3, 1024], P(None, 'tp'), may hold values from -3 to 3
- w_out: bfloat16 [2048, 1024], P(None, 'tp'), may hold values from -0.1875 to 0.1875
Outputs:
- grad_gate: bfloat16 [8, 2048, 1024], P('sp', None, 'tp')
- grad_up: bfloat16 [8, 2048, 1024], P('sp', None, 'tp')
- grad_down: bfloat16 [8, 1024, 2048], P('sp', 'tp')
- out_proj_grad: float32 [2048, 1024], P('sp', 'tp')
- residual_grad: bfloat16 [2048, 2048], P('sp', 'tp')
- grad_b: bfloat16 [2048, 1024], P('sp', 'tp')
- grad_c: bfloat16 [2048, 1024], P('sp', 'tp')
- grad_x: bfloat16 [2048, 1024], P('sp', 'tp')
The draws below stay inside these ranges and needn't reach their ends.
Inputs may be any that keep to these rules, and one draw needn't show every extreme that they name: `routes`: each row names 2 different experts. Among the rows of one index of sp no expert is named more than 96 times, a bound that some block reaches in some of them.
All inputs are finite; a program needn't handle non-finite values.
Results may differ from the reference program's by a relative error of at most 0.01.
Values may be sent and summed in bfloat16 or wider, within the bound.
A program may use at most 64 MiB of HBM per device.

```python
import math
import jax
import jax.numpy as jnp
import numpy as np
from jax import lax

D = 2048
SHORT = 1024
FF = 1024
TOP = 2
TOK_DEV = 256
EXPERTS = 8
CAP = 96
TOKENS = 2048
N_SP = 8
N_TP = 4


def spiked(entries, key, source, target, blocks, factor):
    owner, partner = [(jnp.arange(entries.shape[dim]) // (entries.shape[dim] // blocks)).reshape([-1 if axis == dim else 1 for axis in range(entries.ndim)]) for dim in (source, target)]
    chosen = jax.random.permutation(key, blocks)[partner]
    strong = (owner == chosen) | (owner == (partner + blocks // 2) % blocks)
    return jnp.where(strong, factor * entries, entries)


def shard_levels(own_key, shape, cuts, smallest, largest):
    def one(dim, shards_of):
        heights = jax.random.uniform(jax.random.fold_in(jax.random.fold_in(own_key, 6), dim), (shards_of,), jnp.float32, smallest / len(cuts), largest / len(cuts))
        return jnp.repeat(jnp.exp(heights), shape[dim] // shards_of).reshape((-1,) + (1,) * (len(shape) - dim - 1))

    factor_of = one(*cuts[0])
    for cut in cuts[1:]:
        factor_of = factor_of * one(*cut)
    return factor_of


def routed_block(rng, own, number, rows, amount, top, bound, skew):
    order = jax.random.permutation(rng, amount)
    crowded, ordinary = load_shares(amount, rows * top, bound, skew, True), load_shares(amount, rows * top, bound, skew, False)
    places = jnp.arange(amount)

    def named(sizes, rotation):
        used = int((sizes > 0).sum())
        fixed = max(1, used // 4)
        passed = fixed + (places - fixed + rotation * (used - fixed)) % max(1, amount - fixed)
        return jnp.zeros((amount,), jnp.int32).at[order[jnp.where(places < fixed, places, passed)]].set(jnp.asarray(sizes, jnp.int32))

    sizes = jnp.where(number % 4 == 0, named(crowded, number // 4), named(ordinary, number - number // 4 - 1))
    mixed = jax.random.permutation(jax.random.fold_in(own, 3), amount)
    donor, receiver = mixed[0:amount // 2 * 2:2], mixed[1:amount // 2 * 2:2]
    room = jnp.minimum(sizes[donor] - 1, bound - sizes[receiver]) // 2
    room = jnp.where((donor == order[0]) | (receiver == order[0]) | (sizes[receiver] == 0), 0, jnp.maximum(room, 0))
    passed = jax.random.randint(jax.random.fold_in(own, 4), (amount // 2,), 0, 1 << 20) % (room + 1)
    sizes = sizes.at[donor].add(-passed).at[receiver].add(passed)
    members = jnp.searchsorted(jnp.cumsum(sizes), jnp.arange(rows * top), side="right").astype(jnp.int32)
    table = members.reshape(top, rows).T
    table = table[jax.random.permutation(jax.random.fold_in(own, 1), rows)]
    rotation = jax.random.randint(jax.random.fold_in(own, 2), (rows, 1), 0, top)
    return jnp.take_along_axis(table, (jnp.arange(top)[None, :] + rotation) % top, axis=1)


def load_shares(number_of, total, bound, slope, full):
    weights = [(1 << 20) // math.isqrt(grade ** slope) + 1 for grade in range(1, number_of + 1)]
    largest = bound if full else min(bound, max(-(-total // number_of), total * weights[0] // sum(weights)))
    least = 1 if total - largest >= number_of - 1 else 0
    given, rest = [largest] + [least] * (number_of - 1), total - largest - least * (number_of - 1)
    while rest > 0:
        candidates = [i for i in range(1, number_of) if given[i] < largest] or [i for i in range(1, number_of) if given[i] < bound]
        mass, left = sum([weights[i] for i in candidates]), rest
        for i in candidates:
            more = min(bound - given[i], max(1, left * weights[i] // mass), rest)
            given[i] = given[i] + more
            rest = rest - more
    return np.array(given)


def bell_draw(key, dims, spread, limit, cuts=(), kind=jnp.bfloat16):
    entries = spread * jax.random.normal(key, dims, jnp.float32)
    if cuts:
        entries = entries * shard_levels(key, dims, cuts, -0.22, 0.18)
    return jnp.clip(entries, -limit, limit).astype(kind)


def noise_with(key, dims, deviation, limit, shards, heavy, kind=jnp.bfloat16):
    array = deviation * jax.random.normal(key, dims, jnp.float32)
    if shards:
        array = array * shard_levels(key, dims, shards, -0.22, 0.18)
    return jnp.clip(spiked(array, jax.random.fold_in(key, 3), *heavy), -limit, limit).astype(kind)


def setup_inputs(seed: int = 0) -> dict:
    streams_of = jax.random.split(jax.random.key(seed), 13)
    hidden_in = bell_draw(streams_of[0], (TOKENS, D), 1.0, 6.0, ((0, 8),))
    cotangent = noise_with(streams_of[1], (TOKENS, D), 1.0, 6.0, ((0, 8),), (0, 1, 8, 2.0))
    routes_keys = jax.random.split(jax.random.fold_in(streams_of[2], 1), TOKENS // TOK_DEV)
    routes_turns = jax.random.permutation(jax.random.fold_in(streams_of[2], 3), TOKENS // TOK_DEV)
    routes = jax.vmap(lambda own, number: routed_block(jax.random.fold_in(streams_of[2], 2), own, number, TOK_DEV, EXPERTS, TOP, CAP, 1))(routes_keys, routes_turns).reshape((TOKENS, TOP))
    routing_weights = jnp.clip(jnp.exp(math.log(1.0) - 2.3025851 * jax.random.uniform(streams_of[3], (TOKENS, TOP), jnp.float32) ** shard_levels(streams_of[3], (TOKENS, TOP), ((0, 8),), -0.2, 0.2)), 0.1, 1.0)
    w_gate = bell_draw(streams_of[4], (EXPERTS, D, FF), D ** -0.5, 0.125, ((0, 8), (2, 4)))
    w_up = bell_draw(streams_of[5], (EXPERTS, D, FF), D ** -0.5, 0.125, ((0, 8), (2, 4)))
    w_down = bell_draw(streams_of[6], (EXPERTS, FF, D), FF ** -0.5, 0.1875, ((0, 8), (1, 4)))
    b_gate = bell_draw(streams_of[7], (TOKENS, SHORT), 1.0, 6.0, ((0, 8), (1, 4)))
    c_gate = bell_draw(streams_of[8], (TOKENS, SHORT), 1.0, 6.0, ((0, 8), (1, 4)))
    x_in = bell_draw(streams_of[9], (TOKENS, SHORT), 1.0, 6.0, ((0, 8), (1, 4)))
    taps = bell_draw(streams_of[10], (3, SHORT), 0.6, 3.0, ((1, 4),))
    w_out = bell_draw(streams_of[11], (D, SHORT), SHORT ** -0.5, 0.1875, ((1, 4),))
    return {"hidden_in": hidden_in, "cotangent": cotangent, "routes": routes, "routing_weights": routing_weights, "w_gate": w_gate, "w_up": w_up, "w_down": w_down, "b_gate": b_gate, "c_gate": c_gate, "x_in": x_in, "taps": taps, "w_out": w_out}


def reference(hidden_in, cotangent, routes, routing_weights, w_gate, w_up, w_down, b_gate, c_gate, x_in, taps, w_out):
    flat_ids = routes.reshape(-1).astype(jnp.int32)
    flat_weights = routing_weights.reshape(-1).astype(jnp.float32)
    rows_each = N_SP * CAP
    part_width = FF // N_TP

    def one_expert(args):
        expert_id, gate_mat, up_mat, down_mat = args
        chosen = flat_ids == expert_id
        picked = jnp.nonzero(chosen, size=rows_each, fill_value=0)[0].astype(jnp.int32)
        filled = jnp.arange(rows_each, dtype=jnp.int32) < jnp.sum(chosen.astype(jnp.int32))
        token_of = picked // TOP
        rows_h = jnp.where(filled[:, None], hidden_in[token_of], jnp.zeros((), jnp.bfloat16))
        scaled = jnp.where(filled, flat_weights[picked], 0.0)
        rows_s = (scaled[:, None] * cotangent[token_of].astype(jnp.float32)).astype(jnp.bfloat16)
        pre_gate = jnp.dot(rows_h, gate_mat, preferred_element_type=jnp.float32)
        pre_up = jnp.dot(rows_h, up_mat, preferred_element_type=jnp.float32)
        sigma = jax.nn.sigmoid(pre_gate)
        silu_gate = pre_gate * sigma
        hid = (silu_gate * pre_up).astype(jnp.bfloat16)
        d_hid = jnp.dot(rows_s, down_mat.T, preferred_element_type=jnp.float32)
        d_up = (d_hid * silu_gate).astype(jnp.bfloat16)
        d_pre = (d_hid * pre_up * sigma * (1.0 + pre_gate * (1.0 - sigma))).astype(jnp.bfloat16)
        grad_down_e = jnp.dot(hid.T, rows_s, preferred_element_type=jnp.float32).astype(jnp.bfloat16)
        grad_gate_e = jnp.dot(rows_h.T, d_pre, preferred_element_type=jnp.float32).astype(jnp.bfloat16)
        grad_up_e = jnp.dot(rows_h.T, d_up, preferred_element_type=jnp.float32).astype(jnp.bfloat16)
        total = jnp.zeros((rows_each, D), jnp.float32)
        for block in range(N_TP):
            lower = block * part_width
            upper = lower + part_width
            partial_sum = jnp.dot(d_pre[:, lower:upper], gate_mat[:, lower:upper].T, preferred_element_type=jnp.float32)
            partial_sum = partial_sum + jnp.dot(d_up[:, lower:upper], up_mat[:, lower:upper].T, preferred_element_type=jnp.float32)
            total = total + partial_sum.astype(jnp.bfloat16).astype(jnp.float32)
        route_grad = jnp.where(filled[:, None], total.astype(jnp.bfloat16), jnp.zeros((), jnp.bfloat16))
        return grad_gate_e, grad_up_e, grad_down_e, route_grad, token_of

    expert_ids = jnp.arange(EXPERTS, dtype=jnp.int32)
    grad_gate, grad_up, grad_down, route_grads, token_ids = lax.map(one_expert, (expert_ids, w_gate, w_up, w_down))
    summed = jnp.zeros((TOKENS, D), jnp.float32).at[token_ids.reshape(-1)].add(route_grads.reshape(-1, D).astype(jnp.float32))
    residual_grad = (cotangent.astype(jnp.float32) + summed).astype(jnp.bfloat16)

    taps_f = taps.astype(jnp.float32)
    gated = c_gate.astype(jnp.float32) * x_in.astype(jnp.float32)
    padded = jnp.concatenate([jnp.zeros((2, SHORT), jnp.float32), gated], axis=0)
    conv = taps_f[0] * padded[0:TOKENS] + taps_f[1] * padded[1:TOKENS + 1] + taps_f[2] * padded[2:TOKENS + 2]
    b_f = b_gate.astype(jnp.float32)
    y_short = (b_f * conv).astype(jnp.bfloat16)
    d_y = jnp.dot(residual_grad, w_out, preferred_element_type=jnp.float32)
    grad_b = (d_y * conv).astype(jnp.bfloat16)
    d_conv = b_f * d_y
    later = jnp.concatenate([d_conv, jnp.zeros((2, SHORT), jnp.float32)], axis=0)
    d_v = taps_f[2] * later[0:TOKENS] + taps_f[1] * later[1:TOKENS + 1] + taps_f[0] * later[2:TOKENS + 2]
    grad_c = (d_v * x_in.astype(jnp.float32)).astype(jnp.bfloat16)
    grad_x = (d_v * c_gate.astype(jnp.float32)).astype(jnp.bfloat16)
    out_proj_grad = jnp.dot(residual_grad.T, y_short, preferred_element_type=jnp.float32)
    return grad_gate, grad_up, grad_down, out_proj_grad, residual_grad, grad_b, grad_c, grad_x
```

```python
import functools

import jax
import jax.numpy as jnp
from jax import lax
from jax.experimental import pallas as pl
from jax.experimental.pallas import tpu as pltpu
from jax.sharding import PartitionSpec as P

MESH = pl.DeviceIdType.MESH
BF16, F32 = jnp.bfloat16, jnp.float32
VMEM = pl.BlockSpec(memory_space=pltpu.VMEM)


def coordinates(sp_size, tp_size):
    me, mine = lax.axis_index("sp"), lax.axis_index("tp")
    near = mine + 1 - 2 * (mine % 2)
    far = (mine + tp_size // 2) % tp_size
    return me, mine, near, far


def greet(sp_size, me, tp_partners):
    barrier = pltpu.get_barrier_semaphore()

    def one(i, carry):
        pl.semaphore_signal(
            barrier, inc=1, device_id={"sp": (me + 1 + i) % sp_size}, device_id_type=MESH
        )
        return carry

    lax.fori_loop(0, sp_size - 1, one, 0)
    for partner in tp_partners:
        pl.semaphore_signal(barrier, inc=1, device_id={"tp": partner}, device_id_type=MESH)
    pl.semaphore_wait(barrier, sp_size - 1 + len(tp_partners))


def remote(src, dst, send_sem, recv_sem, to):
    return pltpu.make_async_remote_copy(
        src_ref=src,
        dst_ref=dst,
        send_sem=send_sem,
        recv_sem=recv_sem,
        device_id=to,
        device_id_type=MESH,
    )


def each(count, body):
    def step(i, carry):
        body(i)
        return carry

    lax.fori_loop(0, count, step, 0)


def dispatch_kernel(sp_size, tp_size, send, own, tail, rows, earlier, sems, own_sem, tail_sems):
    me, mine, near, far = coordinates(sp_size, tp_size)
    share = send.shape[3]

    def columns(owner):
        return pl.ds(pl.multiple_of(owner * share, 128), share)

    keep = pltpu.make_async_copy(own, rows.at[:, me], own_sem)
    keep.start()
    greet(sp_size, me, (near, far))
    halo = remote(tail, earlier, tail_sems.at[0], tail_sems.at[1], {"sp": (me + 1) % sp_size})
    halo.start()

    def out(i):
        to = (me + 1 + i) % sp_size
        return remote(
            send.at[:, to],
            rows.at[:, me, :, columns(mine)],
            sems.at[0, i],
            sems.at[1, i],
            {"sp": to},
        )

    def onward(i, owner, lane, partner):
        block = rows.at[:, (me + sp_size - 1 - i) % sp_size, :, columns(owner)]
        return remote(block, block, sems.at[2 * lane, i], sems.at[2 * lane + 1, i], {"tp": partner})

    each(sp_size - 1, lambda i: out(i).start())

    def cross(i):
        onward(i, mine, 1, far).wait_recv()
        onward(i, far, 3, near).start()

    def arrive(i):
        out(i).wait_recv()
        onward(i, mine, 1, far).start()
        onward(i, mine, 2, near).start()
        pl.when(i > 0)(lambda: cross(i - 1))

    each(sp_size - 1, arrive)
    cross(sp_size - 2)

    def finish(i):
        out(i).wait_send()
        onward(i, mine, 1, far).wait_send()
        onward(i, mine, 2, near).wait()
        onward(i, far, 3, near).wait()

    each(sp_size - 1, finish)
    halo.wait()
    keep.wait()


def combine_kernel(
    sp_size,
    tp_size,
    d_pre,
    d_up,
    w_gate,
    w_up,
    place,
    cotangent,
    residual,
    full,
    near_out,
    near_in,
    kept,
    far_out,
    far_in,
    back_out,
    back,
    total,
    sems,
    all_sems,
):
    me, mine, near, far = coordinates(sp_size, tp_size)
    share = residual.shape[1]
    near_far = (near + tp_size // 2) % tp_size
    greet(sp_size, me, (near, far))

    def rows_of(owner):
        return pl.ds(pl.multiple_of(owner * share, 128), share)

    def product(which, owner):
        dims = (((1,), (1,)), ((), ()))
        return lax.dot_general(
            d_pre[which], w_gate[rows_of(owner), :], dims, preferred_element_type=F32
        ) + lax.dot_general(d_up[which], w_up[rows_of(owner), :], dims, preferred_element_type=F32)

    def across(i):
        return remote(near_out.at[i], near_in.at[i], sems.at[0, i], sems.at[1, i], {"tp": near})

    def over(i):
        return remote(far_out.at[i], far_in.at[i], sems.at[2, i], sems.at[3, i], {"tp": far})

    def home(i):
        return remote(
            back_out.at[i],
            back.at[me],
            sems.at[4, i],
            sems.at[5, i],
            {"sp": (me + 1 + i) % sp_size},
        )

    def second(i):
        across(i).wait_recv()
        far_out[i] = (kept[i, 1] + near_in[i, 1].astype(F32)).astype(BF16)
        over(i).start()

    def first(i):
        which = (me + 1 + i) % sp_size
        near_out[i, 0] = product(which, near).astype(BF16)
        near_out[i, 1] = product(which, near_far).astype(BF16)
        across(i).start()
        kept[i, 0] = product(which, mine)
        kept[i, 1] = product(which, far)
        pl.when(i > 0)(lambda: second(i - 1))

    each(sp_size, first)
    second(sp_size - 1)

    def summed(i):
        over(i).wait_recv()
        return (kept[i, 0] + near_in[i, 0].astype(F32) + far_in[i].astype(F32)).astype(BF16)

    def third(i):
        back_out[i] = summed(i)
        home(i).start()

    each(sp_size - 1, third)
    total[...] = cotangent[...].astype(F32) + jnp.dot(
        place[me], summed(sp_size - 1), preferred_element_type=F32
    )

    def collect(i):
        home(i).wait_recv()
        expert = (me + sp_size - 1 - i) % sp_size
        total[...] += jnp.dot(place[expert], back[expert], preferred_element_type=F32)

    each(sp_size - 1, collect)
    result = total[...].astype(BF16)
    residual[...] = result
    full[:, rows_of(mine)] = result

    def gathered(owner, lane, partner):
        block = full.at[:, rows_of(owner)]
        return remote(block, block, all_sems.at[2 * lane], all_sems.at[2 * lane + 1], {"tp": partner})

    to_far, to_near = gathered(mine, 0, far), gathered(mine, 1, near)
    to_far.start()
    to_near.start()
    to_far.wait_recv()
    forward = gathered(far, 2, near)
    forward.start()

    def finish(i):
        across(i).wait_send()
        over(i).wait_send()

    each(sp_size, finish)
    each(sp_size - 1, lambda i: home(i).wait_send())
    to_far.wait_send()
    to_near.wait()
    forward.wait()


def reduce_kernel(sp_size, part, head, out, following, land, sems, head_sems):
    me = lax.axis_index("sp")
    greet(sp_size, me, ())
    halo = remote(
        head, following, head_sems.at[0], head_sems.at[1], {"sp": (me + sp_size - 1) % sp_size}
    )
    halo.start()

    def piece(i):
        to = (me + 1 + i) % sp_size
        return remote(part.at[to], land.at[i], sems.at[0, i], sems.at[1, i], {"sp": to})

    each(sp_size - 1, lambda i: piece(i).start())
    out[...] = part[me].astype(F32)

    def add(i):
        piece(i).wait_recv()
        out[...] += land[i].astype(F32)

    each(sp_size - 1, add)
    each(sp_size - 1, lambda i: piece(i).wait_send())
    halo.wait()


def communicate(kernel, number, inputs, outputs, scratch):
    return pl.pallas_call(
        kernel,
        out_shape=[jax.ShapeDtypeStruct(shape, kind) for shape, kind in outputs],
        in_specs=[VMEM] * len(inputs),
        out_specs=[VMEM] * len(outputs),
        scratch_shapes=scratch,
        compiler_params=pltpu.CompilerParams(collective_id=number, has_side_effects=True),
    )(*inputs)


def per_device(
    hidden_in,
    cotangent,
    routes,
    routing_weights,
    w_gate,
    w_up,
    w_down,
    b_gate,
    c_gate,
    x_in,
    taps,
    w_out,
):
    tok_rows, model_width = hidden_in.shape
    top_k = routes.shape[1]
    sp_size = lax.axis_size("sp")
    tp_size = lax.axis_size("tp")
    experts = w_gate.shape[0] * sp_size
    capacity = 3 * tok_rows * top_k // (2 * experts)
    share = model_width // tp_size
    channels = x_in.shape[1]
    offset = lax.axis_index("tp") * share
    me = lax.axis_index("sp")
    w_gate, w_up, w_down = w_gate[0], w_up[0], w_down[0]

    expert_ids = jnp.arange(experts, dtype=jnp.int32)
    hit = routes[:, :, None] == expert_ids[None, None, :]
    member = jnp.any(hit, axis=1)
    weight = jnp.sum(jnp.where(hit, routing_weights[:, :, None], 0.0), axis=1)
    lower = jnp.tri(tok_rows, k=-1, dtype=BF16)
    position = jnp.dot(lower, member.astype(BF16), preferred_element_type=F32).astype(jnp.int32)
    position = jnp.where(member, position, -1)
    slots = jnp.arange(capacity, dtype=jnp.int32)
    taken = position.T[:, None, :] == slots[None, :, None]
    select = taken.astype(BF16)
    place = (position.T[:, :, None] == slots[None, None, :]).astype(BF16)
    slot_weight = jnp.sum(jnp.where(taken, weight.T[:, None, :], 0.0), axis=2)

    def pick(chosen, weights, rows_src, cot_src):
        rows = jnp.einsum("...t,td->...d", chosen, rows_src, preferred_element_type=F32)
        cot = jnp.einsum("...t,td->...d", chosen, cot_src, preferred_element_type=F32)
        return jnp.stack([rows.astype(BF16), (weights[..., None] * cot).astype(BF16)])

    rows_src = lax.dynamic_slice_in_dim(hidden_in, offset, share, 1)
    cot_src = lax.dynamic_slice_in_dim(cotangent, offset, share, 1)
    send = pick(select, slot_weight, rows_src, cot_src)
    own = pick(select[me], slot_weight[me], hidden_in, cotangent)

    c_f, x_f, b_f = c_gate.astype(F32), x_in.astype(F32), b_gate.astype(F32)
    gated = c_f * x_f
    rows, earlier = communicate(
        functools.partial(dispatch_kernel, sp_size, tp_size),
        0,
        (send, own, gated[tok_rows - 8 :]),
        [((2, sp_size, capacity, model_width), BF16), ((8, channels), F32)],
        [
            pltpu.SemaphoreType.DMA((8, sp_size - 1)),
            pltpu.SemaphoreType.DMA,
            pltpu.SemaphoreType.DMA((2,)),
        ],
    )
    rows_h = rows[0].reshape(sp_size * capacity, model_width)
    rows_s = rows[1].reshape(sp_size * capacity, model_width)

    pre_gate = jnp.dot(rows_h, w_gate, preferred_element_type=F32)
    pre_up = jnp.dot(rows_h, w_up, preferred_element_type=F32)
    sigma = jax.nn.sigmoid(pre_gate)
    silu_gate = pre_gate * sigma
    hid = (silu_gate * pre_up).astype(BF16)
    d_hid = jnp.einsum("rd,fd->rf", rows_s, w_down, preferred_element_type=F32)
    d_up = (d_hid * silu_gate).astype(BF16)
    d_pre = (d_hid * pre_up * sigma * (1.0 + pre_gate * (1.0 - sigma))).astype(BF16)
    grad_down = jnp.einsum("rf,rd->fd", hid, rows_s, preferred_element_type=F32).astype(BF16)
    grad_gate = jnp.einsum("rd,rf->df", rows_h, d_pre, preferred_element_type=F32).astype(BF16)
    grad_up = jnp.einsum("rd,rf->df", rows_h, d_up, preferred_element_type=F32).astype(BF16)

    residual_grad, full_grad = communicate(
        functools.partial(combine_kernel, sp_size, tp_size),
        1,
        (
            d_pre.reshape(sp_size, capacity, -1),
            d_up.reshape(sp_size, capacity, -1),
            w_gate,
            w_up,
            place,
            cot_src,
        ),
        [((tok_rows, share), BF16), ((tok_rows, model_width), BF16)],
        [
            pltpu.VMEM((sp_size, 2, capacity, share), BF16),
            pltpu.VMEM((sp_size, 2, capacity, share), BF16),
            pltpu.VMEM((sp_size, 2, capacity, share), F32),
            pltpu.VMEM((sp_size, capacity, share), BF16),
            pltpu.VMEM((sp_size, capacity, share), BF16),
            pltpu.VMEM((sp_size, capacity, share), BF16),
            pltpu.VMEM((sp_size, capacity, share), BF16),
            pltpu.VMEM((tok_rows, share), F32),
            pltpu.SemaphoreType.DMA((6, sp_size)),
            pltpu.SemaphoreType.DMA((6,)),
        ],
    )

    taps_f = taps.astype(F32)
    earlier = jnp.where(me == 0, 0.0, earlier[6:])
    padded = jnp.concatenate([earlier, gated], axis=0)
    conv = (
        taps_f[0] * padded[0:tok_rows]
        + taps_f[1] * padded[1 : tok_rows + 1]
        + taps_f[2] * padded[2 : tok_rows + 2]
    )
    y_short = (b_f * conv).astype(BF16)
    d_y = jnp.dot(full_grad, w_out, preferred_element_type=F32)
    grad_b = (d_y * conv).astype(BF16)
    d_conv = b_f * d_y
    part = jnp.einsum("td,tc->dc", full_grad, y_short, preferred_element_type=F32).astype(BF16)
    block = model_width // sp_size
    out_proj_grad, following = communicate(
        functools.partial(reduce_kernel, sp_size),
        2,
        (part.reshape(sp_size, block, channels), d_conv[:8]),
        [((block, channels), F32), ((8, channels), F32)],
        [
            pltpu.VMEM((sp_size - 1, block, channels), BF16),
            pltpu.SemaphoreType.DMA((2, sp_size - 1)),
            pltpu.SemaphoreType.DMA((2,)),
        ],
    )
    following = jnp.where(me == sp_size - 1, 0.0, following[:2])
    later = jnp.concatenate([d_conv, following], axis=0)
    d_v = (
        taps_f[2] * later[0:tok_rows]
        + taps_f[1] * later[1 : tok_rows + 1]
        + taps_f[0] * later[2 : tok_rows + 2]
    )
    grad_c = (d_v * x_f).astype(BF16)
    grad_x = (d_v * c_f).astype(BF16)
    grads = (grad_gate[None], grad_up[None], grad_down[None])
    return grads + (out_proj_grad, residual_grad, grad_b, grad_c, grad_x)


def solution(mesh):
    return jax.shard_map(
        per_device,
        mesh=mesh,
        in_specs=(
            P("sp", None),
            P("sp", None),
            P("sp", None),
            P("sp", None),
            P("sp", None, "tp"),
            P("sp", None, "tp"),
            P("sp", "tp", None),
            P("sp", "tp"),
            P("sp", "tp"),
            P("sp", "tp"),
            P(None, "tp"),
            P(None, "tp"),
        ),
        out_specs=(
            P("sp", None, "tp"),
            P("sp", None, "tp"),
            P("sp", "tp", None),
            P("sp", "tp"),
            P("sp", "tp"),
            P("sp", "tp"),
            P("sp", "tp"),
            P("sp", "tp"),
        ),
        check_vma=False,
    )
```

```python
import functools

import jax
import jax.numpy as jnp
from jax import lax
from jax.experimental import pallas as pl
from jax.experimental.pallas import tpu as pltpu
from jax.sharding import PartitionSpec as P

MESH = pl.DeviceIdType.MESH
BF16, F32 = jnp.bfloat16, jnp.float32
VMEM = pl.BlockSpec(memory_space=pltpu.VMEM)
ANY = pl.BlockSpec(memory_space=pl.ANY)


def coordinates(sp_size, tp_size):
    me, mine = lax.axis_index("sp"), lax.axis_index("tp")
    near = mine + 1 - 2 * (mine % 2)
    far = (mine + tp_size // 2) % tp_size
    return me, mine, near, far


def greet(sp_size, me, tp_partners):
    barrier = pltpu.get_barrier_semaphore()

    def one(i, carry):
        pl.semaphore_signal(
            barrier, inc=1, device_id={"sp": (me + 1 + i) % sp_size}, device_id_type=MESH
        )
        return carry

    lax.fori_loop(0, sp_size - 1, one, 0)
    for partner in tp_partners:
        pl.semaphore_signal(barrier, inc=1, device_id={"tp": partner}, device_id_type=MESH)
    pl.semaphore_wait(barrier, sp_size - 1 + len(tp_partners))


def remote(src, dst, send_sem, recv_sem, to):
    return pltpu.make_async_remote_copy(
        src_ref=src,
        dst_ref=dst,
        send_sem=send_sem,
        recv_sem=recv_sem,
        device_id=to,
        device_id_type=MESH,
    )


def each(count, body):
    def step(i, carry):
        body(i)
        return carry

    lax.fori_loop(0, count, step, 0)


def expert_kernel(
    sp_size,
    tp_size,
    send,
    own,
    tail,
    w_gate,
    w_up,
    w_down,
    place,
    cotangent,
    rows_h,
    rows_s,
    hid,
    d_pre,
    d_up,
    residual,
    full,
    earlier,
    rows,
    near_out,
    near_in,
    kept,
    far_out,
    far_in,
    back_out,
    back,
    total,
    row_sems,
    sems,
    save_sems,
    all_sems,
    own_sem,
    tail_sems,
):
    me, mine, near, far = coordinates(sp_size, tp_size)
    share = send.shape[3]
    near_far = (near + tp_size // 2) % tp_size
    last = sp_size - 1

    def columns(owner):
        return pl.ds(pl.multiple_of(owner * share, 128), share)

    def peer(i):
        return (me + sp_size - 1 - i) % sp_size

    keep = pltpu.make_async_copy(own, rows.at[:, me], own_sem)
    keep.start()
    greet(sp_size, me, (near, far))
    halo = remote(tail, earlier, tail_sems.at[0], tail_sems.at[1], {"sp": (me + 1) % sp_size})
    halo.start()

    def out(i):
        to = (me + 1 + i) % sp_size
        return remote(
            send.at[:, to],
            rows.at[:, me, :, columns(mine)],
            row_sems.at[0, i],
            row_sems.at[1, i],
            {"sp": to},
        )

    def onward(i, owner, lane, partner):
        block = rows.at[:, peer(i), :, columns(owner)]
        return remote(
            block, block, row_sems.at[2 * lane, i], row_sems.at[2 * lane + 1, i], {"tp": partner}
        )

    def save(i):
        which = peer(i)
        return (
            pltpu.make_async_copy(rows.at[0, which], rows_h.at[which], save_sems.at[0, i]),
            pltpu.make_async_copy(rows.at[1, which], rows_s.at[which], save_sems.at[1, i]),
        )

    def across(i):
        return remote(near_out.at[i], near_in.at[i], sems.at[0, i], sems.at[1, i], {"tp": near})

    def over(i):
        return remote(far_out.at[i], far_in.at[i], sems.at[2, i], sems.at[3, i], {"tp": far})

    def home(i):
        return remote(
            back_out.at[i], back.at[i], sems.at[4, i], sems.at[5, i], {"sp": peer(i)}
        )

    each(last, lambda i: out(i).start())

    def work(i):
        which = peer(i)
        for copy in save(i):
            copy.start()
        dims = (((1,), (1,)), ((), ()))
        row_h, row_s = rows[0, which], rows[1, which]
        pre_gate = jnp.dot(row_h, w_gate[...], preferred_element_type=F32)
        pre_up = jnp.dot(row_h, w_up[...], preferred_element_type=F32)
        d_hid = lax.dot_general(row_s, w_down[...], dims, preferred_element_type=F32)
        sigma = 1.0 / (1.0 + jnp.exp(-pre_gate))
        silu_gate = pre_gate * sigma
        up = (d_hid * silu_gate).astype(BF16)
        pre = (d_hid * pre_up * sigma * (1.0 + pre_gate * (1.0 - sigma))).astype(BF16)
        hid[which] = (silu_gate * pre_up).astype(BF16)
        d_up[which] = up
        d_pre[which] = pre

        def product(owner):
            return lax.dot_general(
                pre, w_gate[columns(owner), :], dims, preferred_element_type=F32
            ) + lax.dot_general(up, w_up[columns(owner), :], dims, preferred_element_type=F32)

        near_out[i, 0] = product(near).astype(BF16)
        near_out[i, 1] = product(near_far).astype(BF16)
        across(i).start()
        kept[i, 0] = product(mine)
        kept[i, 1] = product(far)

    def second(i):
        across(i).wait_recv()
        far_out[i] = (kept[i, 1] + near_in[i, 1].astype(F32)).astype(BF16)
        over(i).start()

    def summed(i):
        over(i).wait_recv()
        return (kept[i, 0] + near_in[i, 0].astype(F32) + far_in[i].astype(F32)).astype(BF16)

    def arrive(i):
        out(i).wait_recv()
        onward(i, mine, 1, far).start()
        onward(i, mine, 2, near).start()

    def cross(i):
        onward(i, mine, 1, far).wait_recv()
        onward(i, far, 3, near).start()

    def ready(i):
        onward(i, mine, 2, near).wait_recv()
        onward(i, far, 3, near).wait_recv()

    def third(i):
        back_out[i] = summed(i)
        home(i).start()

    def step(i):
        pl.when(i < last)(lambda: arrive(i))
        pl.when((i >= 1) & (i < last + 1))(lambda: cross(i - 1))
        pl.when((i >= 2) & (i < last + 2))(lambda: ready(i - 2))
        pl.when(i == 1)(keep.wait)
        pl.when((i >= 1) & (i < last + 2))(lambda: work((i + last - 1) % sp_size))
        pl.when((i >= 2) & (i < last + 3))(lambda: second((i + last - 2) % sp_size))
        pl.when((i >= 4) & (i < last + 4))(lambda: third(i - 4))

    each(last + 4, step)

    total[...] = cotangent[...].astype(F32) + jnp.dot(
        place[me], summed(last), preferred_element_type=F32
    )

    def collect(i):
        home(i).wait_recv()
        total[...] += jnp.dot(
            place[(me + 1 + i) % sp_size], back[i], preferred_element_type=F32
        )

    each(last, collect)
    result = total[...].astype(BF16)
    residual[...] = result
    full[:, columns(mine)] = result

    def gathered(owner, lane, partner):
        block = full.at[:, columns(owner)]
        return remote(block, block, all_sems.at[2 * lane], all_sems.at[2 * lane + 1], {"tp": partner})

    to_far, to_near = gathered(mine, 0, far), gathered(mine, 1, near)
    to_far.start()
    to_near.start()

    def finish(i):
        across(i).wait_send()
        over(i).wait_send()
        for copy in save(i):
            copy.wait()

    def finish_rows(i):
        out(i).wait_send()
        onward(i, mine, 1, far).wait_send()
        onward(i, mine, 2, near).wait_send()
        onward(i, far, 3, near).wait_send()
        home(i).wait_send()

    each(sp_size, finish)
    each(last, finish_rows)
    halo.wait()
    to_far.wait_recv()
    forward = gathered(far, 2, near)
    forward.start()
    to_far.wait_send()
    to_near.wait()
    forward.wait()


def reduce_kernel(sp_size, part, head, out, following, pair_in, pair_out, land, sems, head_sems):
    me = lax.axis_index("sp")
    side, pair, pairs = me % 2, me // 2, sp_size // 2
    greet(sp_size, me, ())
    halo = remote(
        head, following, head_sems.at[0], head_sems.at[1], {"sp": (me + sp_size - 1) % sp_size}
    )
    halo.start()

    def owner(i):
        return (pair + 1 + i) % pairs

    def beside(i):
        return remote(
            part.at[2 * owner(i) + 1 - side],
            pair_in.at[i],
            sems.at[0, i],
            sems.at[1, i],
            {"sp": me + 1 - 2 * side},
        )

    def along(i):
        return remote(
            pair_out.at[i], land.at[i], sems.at[2, i], sems.at[3, i], {"sp": 2 * owner(i) + side}
        )

    each(pairs, lambda i: beside(i).start())

    def both(i):
        beside(i).wait_recv()
        return part[2 * owner(i) + side].astype(F32) + pair_in[i].astype(F32)

    def onward(i):
        pair_out[i] = both(i).astype(BF16)
        along(i).start()

    each(pairs - 1, onward)
    out[...] = both(pairs - 1)

    def add(i):
        along(i).wait_recv()
        out[...] += land[i].astype(F32)

    each(pairs - 1, add)
    each(pairs, lambda i: beside(i).wait_send())
    each(pairs - 1, lambda i: along(i).wait_send())
    halo.wait()


def communicate(kernel, number, inputs, outputs, scratch, unplaced=0):
    return pl.pallas_call(
        kernel,
        out_shape=[jax.ShapeDtypeStruct(shape, kind) for shape, kind in outputs],
        in_specs=[VMEM] * len(inputs),
        out_specs=[ANY] * unplaced + [VMEM] * (len(outputs) - unplaced),
        scratch_shapes=scratch,
        compiler_params=pltpu.CompilerParams(collective_id=number, has_side_effects=True),
    )(*inputs)


def per_device(
    hidden_in,
    cotangent,
    routes,
    routing_weights,
    w_gate,
    w_up,
    w_down,
    b_gate,
    c_gate,
    x_in,
    taps,
    w_out,
):
    tok_rows, model_width = hidden_in.shape
    top_k = routes.shape[1]
    sp_size = lax.axis_size("sp")
    tp_size = lax.axis_size("tp")
    experts = w_gate.shape[0] * sp_size
    capacity = 3 * tok_rows * top_k // (2 * experts)
    share = model_width // tp_size
    channels = x_in.shape[1]
    offset = lax.axis_index("tp") * share
    me = lax.axis_index("sp")
    w_gate, w_up, w_down = w_gate[0], w_up[0], w_down[0]

    expert_ids = jnp.arange(experts, dtype=jnp.int32)
    hit = routes[:, :, None] == expert_ids[None, None, :]
    member = jnp.any(hit, axis=1)
    weight = jnp.sum(jnp.where(hit, routing_weights[:, :, None], 0.0), axis=1)
    lower = jnp.tri(tok_rows, k=-1, dtype=BF16)
    position = jnp.dot(lower, member.astype(BF16), preferred_element_type=F32).astype(jnp.int32)
    position = jnp.where(member, position, -1)
    slots = jnp.arange(capacity, dtype=jnp.int32)
    taken = position.T[:, None, :] == slots[None, :, None]
    select = taken.astype(BF16)
    place = (position.T[:, :, None] == slots[None, None, :]).astype(BF16)
    slot_weight = jnp.sum(jnp.where(taken, weight.T[:, None, :], 0.0), axis=2)

    def pick(chosen, weights, rows_src, cot_src):
        rows = jnp.einsum("...t,td->...d", chosen, rows_src, preferred_element_type=F32)
        cot = jnp.einsum("...t,td->...d", chosen, cot_src, preferred_element_type=F32)
        return jnp.stack([rows.astype(BF16), (weights[..., None] * cot).astype(BF16)])

    rows_src = lax.dynamic_slice_in_dim(hidden_in, offset, share, 1)
    cot_src = lax.dynamic_slice_in_dim(cotangent, offset, share, 1)
    send = pick(select, slot_weight, rows_src, cot_src)
    own = pick(select[me], slot_weight[me], hidden_in, cotangent)

    c_f, x_f, b_f = c_gate.astype(F32), x_in.astype(F32), b_gate.astype(F32)
    gated = c_f * x_f
    hidden = w_gate.shape[1]
    row_shape, hid_shape = (sp_size, capacity, model_width), (sp_size, capacity, hidden)
    rows_h, rows_s, hid, d_pre, d_up, residual_grad, full_grad, earlier = communicate(
        functools.partial(expert_kernel, sp_size, tp_size),
        0,
        (send, own, gated[tok_rows - 8 :], w_gate, w_up, w_down, place, cot_src),
        [(row_shape, BF16)] * 2
        + [(hid_shape, BF16)] * 3
        + [((tok_rows, share), BF16), ((tok_rows, model_width), BF16), ((8, channels), F32)],
        [
            pltpu.VMEM((2, sp_size, capacity, model_width), BF16),
            pltpu.VMEM((sp_size, 2, capacity, share), BF16),
            pltpu.VMEM((sp_size, 2, capacity, share), BF16),
            pltpu.VMEM((sp_size, 2, capacity, share), F32),
            pltpu.VMEM((sp_size, capacity, share), BF16),
            pltpu.VMEM((sp_size, capacity, share), BF16),
            pltpu.VMEM((sp_size - 1, capacity, share), BF16),
            pltpu.VMEM((sp_size - 1, capacity, share), BF16),
            pltpu.VMEM((tok_rows, share), F32),
            pltpu.SemaphoreType.DMA((8, sp_size - 1)),
            pltpu.SemaphoreType.DMA((6, sp_size)),
            pltpu.SemaphoreType.DMA((2, sp_size)),
            pltpu.SemaphoreType.DMA((6,)),
            pltpu.SemaphoreType.DMA,
            pltpu.SemaphoreType.DMA((2,)),
        ],
        unplaced=2,
    )
    flat = sp_size * capacity
    rows_h, rows_s = rows_h.reshape(flat, model_width), rows_s.reshape(flat, model_width)
    hid, d_pre, d_up = (a.reshape(flat, hidden) for a in (hid, d_pre, d_up))
    grad_down = jnp.einsum("rf,rd->fd", hid, rows_s, preferred_element_type=F32).astype(BF16)
    grad_gate = jnp.einsum("rd,rf->df", rows_h, d_pre, preferred_element_type=F32).astype(BF16)
    grad_up = jnp.einsum("rd,rf->df", rows_h, d_up, preferred_element_type=F32).astype(BF16)

    taps_f = taps.astype(F32)
    earlier = jnp.where(me == 0, 0.0, earlier[6:])
    padded = jnp.concatenate([earlier, gated], axis=0)
    conv = (
        taps_f[0] * padded[0:tok_rows]
        + taps_f[1] * padded[1 : tok_rows + 1]
        + taps_f[2] * padded[2 : tok_rows + 2]
    )
    y_short = (b_f * conv).astype(BF16)
    d_y = jnp.dot(full_grad, w_out, preferred_element_type=F32)
    grad_b = (d_y * conv).astype(BF16)
    d_conv = b_f * d_y
    part = jnp.einsum("td,tc->dc", full_grad, y_short, preferred_element_type=F32).astype(BF16)
    block = model_width // sp_size
    out_proj_grad, following = communicate(
        functools.partial(reduce_kernel, sp_size),
        1,
        (part.reshape(sp_size, block, channels), d_conv[:8]),
        [((block, channels), F32), ((8, channels), F32)],
        [
            pltpu.VMEM((sp_size // 2, block, channels), BF16),
            pltpu.VMEM((sp_size // 2, block, channels), BF16),
            pltpu.VMEM((sp_size // 2, block, channels), BF16),
            pltpu.SemaphoreType.DMA((4, sp_size // 2)),
            pltpu.SemaphoreType.DMA((2,)),
        ],
    )
    following = jnp.where(me == sp_size - 1, 0.0, following[:2])
    later = jnp.concatenate([d_conv, following], axis=0)
    d_v = (
        taps_f[2] * later[0:tok_rows]
        + taps_f[1] * later[1 : tok_rows + 1]
        + taps_f[0] * later[2 : tok_rows + 2]
    )
    grad_c = (d_v * x_f).astype(BF16)
    grad_x = (d_v * c_f).astype(BF16)
    grads = (grad_gate[None], grad_up[None], grad_down[None])
    return grads + (out_proj_grad, residual_grad, grad_b, grad_c, grad_x)


def solution(mesh):
    return jax.shard_map(
        per_device,
        mesh=mesh,
        in_specs=(
            P("sp", None),
            P("sp", None),
            P("sp", None),
            P("sp", None),
            P("sp", None, "tp"),
            P("sp", None, "tp"),
            P("sp", "tp", None),
            P("sp", "tp"),
            P("sp", "tp"),
            P("sp", "tp"),
            P(None, "tp"),
            P(None, "tp"),
        ),
        out_specs=(
            P("sp", None, "tp"),
            P("sp", None, "tp"),
            P("sp", "tp", None),
            P("sp", "tp"),
            P("sp", "tp"),
            P("sp", "tp"),
            P("sp", "tp"),
            P("sp", "tp"),
        ),
        check_vma=False,
    )
```

```python
import functools

import jax
import jax.numpy as jnp
from jax import lax
from jax.experimental import pallas as pl
from jax.experimental.pallas import tpu as pltpu
from jax.sharding import PartitionSpec as P

MESH = pl.DeviceIdType.MESH
BF16, F32 = jnp.bfloat16, jnp.float32
VMEM = pl.BlockSpec(memory_space=pltpu.VMEM)
ANY = pl.BlockSpec(memory_space=pl.ANY)


def coordinates(sp_size, tp_size):
    me, mine = lax.axis_index("sp"), lax.axis_index("tp")
    near = mine + 1 - 2 * (mine % 2)
    far = (mine + tp_size // 2) % tp_size
    return me, mine, near, far


def greet(sp_size, me, tp_partners):
    barrier = pltpu.get_barrier_semaphore()

    def one(i, carry):
        pl.semaphore_signal(
            barrier, inc=1, device_id={"sp": (me + 1 + i) % sp_size}, device_id_type=MESH
        )
        return carry

    lax.fori_loop(0, sp_size - 1, one, 0)
    for partner in tp_partners:
        pl.semaphore_signal(barrier, inc=1, device_id={"tp": partner}, device_id_type=MESH)
    pl.semaphore_wait(barrier, sp_size - 1 + len(tp_partners))


def remote(src, dst, send_sem, recv_sem, to):
    return pltpu.make_async_remote_copy(
        src_ref=src,
        dst_ref=dst,
        send_sem=send_sem,
        recv_sem=recv_sem,
        device_id=to,
        device_id_type=MESH,
    )


def each(count, body):
    def step(i, carry):
        body(i)
        return carry

    lax.fori_loop(0, count, step, 0)


def expert_kernel(
    sp_size,
    tp_size,
    send,
    own,
    tail,
    w_gate,
    w_up,
    w_down,
    place,
    cotangent,
    rows_h,
    rows_s,
    hid,
    d_pre,
    d_up,
    residual,
    full,
    earlier,
    rows,
    near_out,
    near_in,
    kept,
    far_out,
    far_in,
    back_out,
    back,
    total,
    row_sems,
    sems,
    save_sems,
    all_sems,
    own_sem,
    tail_sems,
):
    me, mine, near, far = coordinates(sp_size, tp_size)
    share = send.shape[3]
    near_far = (near + tp_size // 2) % tp_size
    last = sp_size - 1

    def columns(owner):
        return pl.ds(pl.multiple_of(owner * share, 128), share)

    def peer(i):
        mask = ((i + 1) * 3) % sp_size
        other, bit = me, 1
        while bit < sp_size:
            other = other + ((mask // bit) % 2) * bit * (1 - 2 * ((me // bit) % 2))
            bit *= 2
        return other

    keep = pltpu.make_async_copy(own, rows.at[:, me], own_sem)
    keep.start()
    greet(sp_size, me, (near, far))
    halo = remote(tail, earlier, tail_sems.at[0], tail_sems.at[1], {"sp": (me + 1) % sp_size})
    halo.start()

    def out(i):
        to = peer(i)
        return remote(
            send.at[:, to],
            rows.at[:, me, :, columns(mine)],
            row_sems.at[0, i],
            row_sems.at[1, i],
            {"sp": to},
        )

    def onward(i, owner, lane, partner):
        block = rows.at[:, peer(i), :, columns(owner)]
        return remote(
            block, block, row_sems.at[2 * lane, i], row_sems.at[2 * lane + 1, i], {"tp": partner}
        )

    def save(i):
        which = peer(i)
        return (
            pltpu.make_async_copy(rows.at[0, which], rows_h.at[which], save_sems.at[0, i]),
            pltpu.make_async_copy(rows.at[1, which], rows_s.at[which], save_sems.at[1, i]),
        )

    def across(i):
        return remote(near_out.at[i], near_in.at[i], sems.at[0, i], sems.at[1, i], {"tp": near})

    def over(i):
        return remote(far_out.at[i], far_in.at[i], sems.at[2, i], sems.at[3, i], {"tp": far})

    def home(i):
        return remote(
            back_out.at[i], back.at[i], sems.at[4, i], sems.at[5, i], {"sp": peer(i)}
        )

    each(last, lambda i: out(i).start())

    def work(i):
        which = peer(i)
        for copy in save(i):
            copy.start()
        dims = (((1,), (1,)), ((), ()))
        row_h, row_s = rows[0, which], rows[1, which]
        pre_gate = jnp.dot(row_h, w_gate[...], preferred_element_type=F32)
        pre_up = jnp.dot(row_h, w_up[...], preferred_element_type=F32)
        d_hid = lax.dot_general(row_s, w_down[...], dims, preferred_element_type=F32)
        sigma = 1.0 / (1.0 + jnp.exp(-pre_gate))
        silu_gate = pre_gate * sigma
        up = (d_hid * silu_gate).astype(BF16)
        pre = (d_hid * pre_up * sigma * (1.0 + pre_gate * (1.0 - sigma))).astype(BF16)
        hid[which] = (silu_gate * pre_up).astype(BF16)
        d_up[which] = up
        d_pre[which] = pre

        def product(owner):
            return lax.dot_general(
                pre, w_gate[columns(owner), :], dims, preferred_element_type=F32
            ) + lax.dot_general(up, w_up[columns(owner), :], dims, preferred_element_type=F32)

        near_out[i, 0] = product(near).astype(BF16)
        near_out[i, 1] = product(near_far).astype(BF16)
        across(i).start()
        kept[i, 0] = product(mine)
        kept[i, 1] = product(far)

    def second(i):
        across(i).wait_recv()
        far_out[i] = (kept[i, 1] + near_in[i, 1].astype(F32)).astype(BF16)
        over(i).start()

    def summed(i):
        over(i).wait_recv()
        return (kept[i, 0] + near_in[i, 0].astype(F32) + far_in[i].astype(F32)).astype(BF16)

    def arrive(i):
        out(i).wait_recv()
        onward(i, mine, 1, far).start()
        onward(i, mine, 2, near).start()

    def cross(i):
        onward(i, mine, 1, far).wait_recv()
        onward(i, far, 3, near).start()

    def ready(i):
        onward(i, mine, 2, near).wait_recv()
        onward(i, far, 3, near).wait_recv()

    def third(i):
        back_out[i] = summed(i)
        home(i).start()

    def step(i):
        pl.when(i < last)(lambda: arrive(i))
        pl.when((i >= 1) & (i < last + 1))(lambda: cross(i - 1))
        pl.when((i >= 2) & (i < last + 2))(lambda: ready(i - 2))
        pl.when(i == 1)(keep.wait)
        pl.when((i >= 1) & (i < last + 2))(lambda: work((i + last - 1) % sp_size))
        pl.when((i >= 2) & (i < last + 3))(lambda: second((i + last - 2) % sp_size))
        pl.when((i >= 4) & (i < last + 4))(lambda: third(i - 4))

    each(last + 4, step)

    total[...] = cotangent[...].astype(F32) + jnp.dot(
        place[me], summed(last), preferred_element_type=F32
    )

    def collect(i):
        home(i).wait_recv()
        total[...] += jnp.dot(
            place[peer(i)], back[i], preferred_element_type=F32
        )

    each(last, collect)
    result = total[...].astype(BF16)
    residual[...] = result
    full[:, columns(mine)] = result

    def gathered(owner, lane, partner):
        block = full.at[:, columns(owner)]
        return remote(block, block, all_sems.at[2 * lane], all_sems.at[2 * lane + 1], {"tp": partner})

    to_far, to_near = gathered(mine, 0, far), gathered(mine, 1, near)
    to_far.start()
    to_near.start()

    def finish(i):
        across(i).wait_send()
        over(i).wait_send()
        for copy in save(i):
            copy.wait()

    def finish_rows(i):
        out(i).wait_send()
        onward(i, mine, 1, far).wait_send()
        onward(i, mine, 2, near).wait_send()
        onward(i, far, 3, near).wait_send()
        home(i).wait_send()

    each(sp_size, finish)
    each(last, finish_rows)
    halo.wait()
    to_far.wait_recv()
    forward = gathered(far, 2, near)
    forward.start()
    to_far.wait_send()
    to_near.wait()
    forward.wait()


def reduce_kernel(sp_size, part, head, out, following, pair_in, pair_out, land, sems, head_sems):
    me = lax.axis_index("sp")
    side, pair, pairs = me % 2, me // 2, sp_size // 2
    greet(sp_size, me, ())
    halo = remote(
        head, following, head_sems.at[0], head_sems.at[1], {"sp": (me + sp_size - 1) % sp_size}
    )
    halo.start()

    def owner(i):
        return (pair + 1 + i) % pairs

    def beside(i):
        return remote(
            part.at[2 * owner(i) + 1 - side],
            pair_in.at[i],
            sems.at[0, i],
            sems.at[1, i],
            {"sp": me + 1 - 2 * side},
        )

    def along(i):
        return remote(
            pair_out.at[i], land.at[i], sems.at[2, i], sems.at[3, i], {"sp": 2 * owner(i) + side}
        )

    each(pairs, lambda i: beside(i).start())

    def both(i):
        beside(i).wait_recv()
        return part[2 * owner(i) + side].astype(F32) + pair_in[i].astype(F32)

    def onward(i):
        pair_out[i] = both(i).astype(BF16)
        along(i).start()

    each(pairs - 1, onward)
    out[...] = both(pairs - 1)

    def add(i):
        along(i).wait_recv()
        out[...] += land[i].astype(F32)

    each(pairs - 1, add)
    each(pairs, lambda i: beside(i).wait_send())
    each(pairs - 1, lambda i: along(i).wait_send())
    halo.wait()


def communicate(kernel, number, inputs, outputs, scratch, unplaced=0):
    return pl.pallas_call(
        kernel,
        out_shape=[jax.ShapeDtypeStruct(shape, kind) for shape, kind in outputs],
        in_specs=[VMEM] * len(inputs),
        out_specs=[ANY] * unplaced + [VMEM] * (len(outputs) - unplaced),
        scratch_shapes=scratch,
        compiler_params=pltpu.CompilerParams(collective_id=number, has_side_effects=True),
    )(*inputs)


def per_device(
    hidden_in,
    cotangent,
    routes,
    routing_weights,
    w_gate,
    w_up,
    w_down,
    b_gate,
    c_gate,
    x_in,
    taps,
    w_out,
):
    tok_rows, model_width = hidden_in.shape
    top_k = routes.shape[1]
    sp_size = lax.axis_size("sp")
    tp_size = lax.axis_size("tp")
    experts = w_gate.shape[0] * sp_size
    capacity = 3 * tok_rows * top_k // (2 * experts)
    share = model_width // tp_size
    channels = x_in.shape[1]
    offset = lax.axis_index("tp") * share
    me = lax.axis_index("sp")
    w_gate, w_up, w_down = w_gate[0], w_up[0], w_down[0]

    expert_ids = jnp.arange(experts, dtype=jnp.int32)
    hit = routes[:, :, None] == expert_ids[None, None, :]
    member = jnp.any(hit, axis=1)
    weight = jnp.sum(jnp.where(hit, routing_weights[:, :, None], 0.0), axis=1)
    lower = jnp.tri(tok_rows, k=-1, dtype=BF16)
    position = jnp.dot(lower, member.astype(BF16), preferred_element_type=F32).astype(jnp.int32)
    position = jnp.where(member, position, -1)
    slots = jnp.arange(capacity, dtype=jnp.int32)
    taken = position.T[:, None, :] == slots[None, :, None]
    select = taken.astype(BF16)
    place = (position.T[:, :, None] == slots[None, None, :]).astype(BF16)
    slot_weight = jnp.sum(jnp.where(taken, weight.T[:, None, :], 0.0), axis=2)

    def pick(chosen, weights, rows_src, cot_src):
        rows = jnp.einsum("...t,td->...d", chosen, rows_src, preferred_element_type=F32)
        cot = jnp.einsum("...t,td->...d", chosen, cot_src, preferred_element_type=F32)
        return jnp.stack([rows.astype(BF16), (weights[..., None] * cot).astype(BF16)])

    rows_src = lax.dynamic_slice_in_dim(hidden_in, offset, share, 1)
    cot_src = lax.dynamic_slice_in_dim(cotangent, offset, share, 1)
    send = pick(select, slot_weight, rows_src, cot_src)
    own = pick(select[me], slot_weight[me], hidden_in, cotangent)

    c_f, x_f, b_f = c_gate.astype(F32), x_in.astype(F32), b_gate.astype(F32)
    gated = c_f * x_f
    hidden = w_gate.shape[1]
    row_shape, hid_shape = (sp_size, capacity, model_width), (sp_size, capacity, hidden)
    rows_h, rows_s, hid, d_pre, d_up, residual_grad, full_grad, earlier = communicate(
        functools.partial(expert_kernel, sp_size, tp_size),
        0,
        (send, own, gated[tok_rows - 8 :], w_gate, w_up, w_down, place, cot_src),
        [(row_shape, BF16)] * 2
        + [(hid_shape, BF16)] * 3
        + [((tok_rows, share), BF16), ((tok_rows, model_width), BF16), ((8, channels), F32)],
        [
            pltpu.VMEM((2, sp_size, capacity, model_width), BF16),
            pltpu.VMEM((sp_size, 2, capacity, share), BF16),
            pltpu.VMEM((sp_size, 2, capacity, share), BF16),
            pltpu.VMEM((sp_size, 2, capacity, share), F32),
            pltpu.VMEM((sp_size, capacity, share), BF16),
            pltpu.VMEM((sp_size, capacity, share), BF16),
            pltpu.VMEM((sp_size - 1, capacity, share), BF16),
            pltpu.VMEM((sp_size - 1, capacity, share), BF16),
            pltpu.VMEM((tok_rows, share), F32),
            pltpu.SemaphoreType.DMA((8, sp_size - 1)),
            pltpu.SemaphoreType.DMA((6, sp_size)),
            pltpu.SemaphoreType.DMA((2, sp_size)),
            pltpu.SemaphoreType.DMA((6,)),
            pltpu.SemaphoreType.DMA,
            pltpu.SemaphoreType.DMA((2,)),
        ],
        unplaced=2,
    )
    flat = sp_size * capacity
    rows_h, rows_s = rows_h.reshape(flat, model_width), rows_s.reshape(flat, model_width)
    hid, d_pre, d_up = (a.reshape(flat, hidden) for a in (hid, d_pre, d_up))
    grad_down = jnp.einsum("rf,rd->fd", hid, rows_s, preferred_element_type=F32).astype(BF16)
    grad_gate = jnp.einsum("rd,rf->df", rows_h, d_pre, preferred_element_type=F32).astype(BF16)
    grad_up = jnp.einsum("rd,rf->df", rows_h, d_up, preferred_element_type=F32).astype(BF16)

    taps_f = taps.astype(F32)
    earlier = jnp.where(me == 0, 0.0, earlier[6:])
    padded = jnp.concatenate([earlier, gated], axis=0)
    conv = (
        taps_f[0] * padded[0:tok_rows]
        + taps_f[1] * padded[1 : tok_rows + 1]
        + taps_f[2] * padded[2 : tok_rows + 2]
    )
    y_short = (b_f * conv).astype(BF16)
    d_y = jnp.dot(full_grad, w_out, preferred_element_type=F32)
    grad_b = (d_y * conv).astype(BF16)
    d_conv = b_f * d_y
    part = jnp.einsum("td,tc->dc", full_grad, y_short, preferred_element_type=F32).astype(BF16)
    block = model_width // sp_size
    out_proj_grad, following = communicate(
        functools.partial(reduce_kernel, sp_size),
        1,
        (part.reshape(sp_size, block, channels), d_conv[:8]),
        [((block, channels), F32), ((8, channels), F32)],
        [
            pltpu.VMEM((sp_size // 2, block, channels), BF16),
            pltpu.VMEM((sp_size // 2, block, channels), BF16),
            pltpu.VMEM((sp_size // 2, block, channels), BF16),
            pltpu.SemaphoreType.DMA((4, sp_size // 2)),
            pltpu.SemaphoreType.DMA((2,)),
        ],
    )
    following = jnp.where(me == sp_size - 1, 0.0, following[:2])
    later = jnp.concatenate([d_conv, following], axis=0)
    d_v = (
        taps_f[2] * later[0:tok_rows]
        + taps_f[1] * later[1 : tok_rows + 1]
        + taps_f[0] * later[2 : tok_rows + 2]
    )
    grad_c = (d_v * x_f).astype(BF16)
    grad_x = (d_v * c_f).astype(BF16)
    grads = (grad_gate[None], grad_up[None], grad_down[None])
    return grads + (out_proj_grad, residual_grad, grad_b, grad_c, grad_x)


def solution(mesh):
    return jax.shard_map(
        per_device,
        mesh=mesh,
        in_specs=(
            P("sp", None),
            P("sp", None),
            P("sp", None),
            P("sp", None),
            P("sp", None, "tp"),
            P("sp", None, "tp"),
            P("sp", "tp", None),
            P("sp", "tp"),
            P("sp", "tp"),
            P("sp", "tp"),
            P(None, "tp"),
            P(None, "tp"),
        ),
        out_specs=(
            P("sp", None, "tp"),
            P("sp", None, "tp"),
            P("sp", "tp", None),
            P("sp", "tp"),
            P("sp", "tp"),
            P("sp", "tp"),
            P("sp", "tp"),
            P("sp", "tp"),
        ),
        check_vma=False,
    )
```
